32 devices in a mesh: sp: 8 (over z, x), dp: 4 (over y, core).
Axes of the slice: x: 2, y: 2, z: 4, core: 2. Of those that a mesh axis runs over, the one named last changes fastest.
Arguments:
- tokens: bfloat16 [4, 4096, 2048], P('dp', 'sp'), may hold values from -6 to 6
- segments: int32 [4, 4096], P('dp', 'sp'), may hold values from 0 to 3, never falling along the last dimension, each value on 1 to 2048 neighbouring positions
- w_lin: bfloat16 [2048, 1024], P('dp'), may hold values from -0.125 to 0.125
- w_gate: bfloat16 [2048, 1024], P('dp'), may hold values from -0.125 to 0.125
- w_out: bfloat16 [1024, 2048], P(None, 'dp'), may hold values from -0.1875 to 0.1875
- conv_kernel: float32 [31, 1024], replicated, may hold values from -1 to 1
- conv_bias: float32 [1024], replicated, may hold values from -3 to 3
- norm_gain: float32 [1024], replicated, may hold values from 0.1 to 1.9
- norm_bias: float32 [1024], replicated, may hold values from -3 to 3
Outputs:
- mixed_out: bfloat16 [4, 4096, 2048], P('dp', 'sp')
The draws below stay inside these ranges and needn't reach their ends.
Inputs may be any that keep to these rules, and one draw needn't show every extreme that they name: `segments`: within each sequence document numbers never fall; a document is a run of equal numbers of at most four times 512 positions.
All inputs are finite; a program needn't handle non-finite values.
Results may differ from the reference program's by a relative error of at most 0.0062.
Values may be sent and summed in bfloat16 or wider, within the bound.
A program may use at most 64 MiB of HBM per device.

```python
import math
import jax
import jax.numpy as jnp
import numpy as np
from jax import lax

D = 2048
CW = 1024
K = 31
TOK_DEV = 512
SEQ = 4096
SEQS = 4
N_SP = 8


def steps_of(stream_key, shape, cuts, least, high):
    factor_of, own = 1.0, jax.random.fold_in(stream_key, 6)
    for axis_at, parts in cuts:
        heights = jnp.exp(jax.random.uniform(jax.random.fold_in(own, axis_at), (parts,), jnp.float32, least / len(cuts), high / len(cuts)))
        factor_of = factor_of * jnp.repeat(heights, shape[axis_at] // parts).reshape([-1 if axis == axis_at else 1 for axis in range(len(shape))])
    return factor_of


def length_profile(number_of, total, reach, slope):
    weights = [(1 << 20) // math.isqrt(grade ** slope) + 1 for grade in range(2, number_of + 1)]
    spare, holding = total - reach - (number_of - 1), [1] * (number_of - 1)
    while spare > 0:
        candidates = [i for i in range(number_of - 1) if holding[i] < reach]
        whole, remaining = sum([weights[i] for i in candidates]), spare
        for i in candidates:
            extra = min(reach - holding[i], max(1, remaining * weights[i] // whole), spare)
            holding[i] = holding[i] + extra
            spare = spare - extra
    return np.array([reach] + holding)


def uneven_parts(own_key, count, total, bound, lean):
    if count == 2:
        one = jax.random.randint(own_key, (), max(1, total - bound), min(bound, total - 1) + 1)
        return jnp.stack([one, total - one])
    sizes = jnp.asarray(length_profile(count, total, bound, lean), jnp.int32)
    couples = (count - 1) // 2
    source_of, receiver = sizes[1:1 + 2 * couples:2], sizes[2:2 + 2 * couples:2]
    room = jnp.minimum(source_of - 1, bound - receiver)
    moved = jax.random.randint(jax.random.fold_in(own_key, 1), (couples,), 0, 1 << 20) % (room + 1)
    sizes = sizes.at[1:1 + 2 * couples:2].set(source_of - moved).at[2:2 + 2 * couples:2].set(receiver + moved)
    return sizes[jax.random.permutation(jax.random.fold_in(own_key, 2), count)]


def normal_values(rng, dims, width, limit, cuts=(), held_as=jnp.bfloat16):
    drawn = width * jax.random.normal(rng, dims, jnp.float32)
    if cuts:
        drawn = drawn * steps_of(rng, dims, cuts, -0.22, 0.18)
    return jnp.clip(drawn, -limit, limit).astype(held_as)


def setup_inputs(seed: int = 0) -> dict:
    streams_of = jax.random.split(jax.random.key(seed), 10)
    return {
        "tokens": normal_values(streams_of[0], (SEQS, SEQ, D), 1.0, 6.0, ((0, 4), (1, 8))),
        "segments": jax.vmap(lambda own: jnp.searchsorted(jnp.cumsum(uneven_parts(own, N_SP // 2, SEQ, 4 * TOK_DEV, 2)), jnp.arange(SEQ), side="right"))(jax.random.split(streams_of[1], SEQS)).reshape((SEQS, SEQ)).astype(jnp.int32),
        "w_lin": normal_values(streams_of[2], (D, CW), D ** -0.5, 0.125, ((0, 4),)),
        "w_gate": normal_values(streams_of[3], (D, CW), D ** -0.5, 0.125, ((0, 4),)),
        "w_out": normal_values(streams_of[4], (CW, D), CW ** -0.5, 0.1875, ((1, 4),)),
        "conv_kernel": normal_values(streams_of[5], (K, CW), K ** -0.5, 1.0, (), jnp.float32),
        "conv_bias": normal_values(streams_of[6], (CW,), 0.5, 3.0, (), jnp.float32),
        "norm_gain": jnp.clip(1.0 + 0.18 * jax.random.normal(streams_of[7], (CW,), jnp.float32), 0.1, 1.9),
        "norm_bias": normal_values(streams_of[8], (CW,), 0.5, 3.0, (), jnp.float32),
    }


def conv_doc(values, doc_ids, kernel, bias):
    length = values.shape[1]
    taps = kernel.shape[0]
    total = bias[:, None] + kernel[taps - 1][:, None] * values
    for back in range(1, taps):
        shifted = jnp.pad(values[:, :length - back], ((0, 0), (back, 0)))
        same = jnp.pad(doc_ids[back:] == doc_ids[:length - back], (back, 0))
        total = total + kernel[taps - 1 - back][:, None] * jnp.where(same[None, :], shifted, 0.0)
    return total

def reference(tokens, segments, w_lin, w_gate, w_out, conv_kernel, conv_bias, norm_gain, norm_bias):

    def one_sequence(pair):
        rows, doc_ids = pair
        lin = jnp.dot(rows, w_lin, preferred_element_type=jnp.float32)
        gate = jnp.dot(rows, w_gate, preferred_element_type=jnp.float32)
        glu = (lin * jax.nn.sigmoid(gate)).astype(jnp.bfloat16)
        conv = conv_doc(glu.T.astype(jnp.float32), doc_ids, conv_kernel, conv_bias)
        values = lax.optimization_barrier(conv.astype(jnp.bfloat16)).astype(jnp.float32)
        mean = lax.optimization_barrier(jnp.mean(values, axis=0, keepdims=True))
        var = lax.optimization_barrier(jnp.mean(jnp.square(values - mean), axis=0, keepdims=True))
        normed = (values - mean) * lax.rsqrt(var + 1e-05) * norm_gain[:, None] + norm_bias[:, None]
        act = jax.nn.silu(normed).astype(jnp.bfloat16)
        return jnp.dot(act.T, w_out, preferred_element_type=jnp.float32).astype(jnp.bfloat16)
    return lax.map(one_sequence, (tokens, segments))
```

```python
import functools

import jax
import jax.numpy as jnp
from jax import lax
from jax.experimental import pallas as pl
from jax.experimental.pallas import tpu as pltpu
from jax.sharding import PartitionSpec as P

MESH = pl.DeviceIdType.MESH
BLK = 256
LANES = 128


def from_behind(value, axis, by):
    devices = lax.axis_size(axis)
    pairs = [(i, i + by) for i in range(devices) if 0 <= i + by < devices]
    return lax.ppermute(value, axis, pairs)


def conv_doc(values, doc_ids, kernel, bias):
    taps = kernel.shape[0]
    reach = taps - 1
    length = values.shape[1]
    place = lax.iota(jnp.int32, length)
    change = jnp.concatenate([jnp.ones((1,), jnp.bool_), doc_ids[1:] != doc_ids[:-1]])
    begins = lax.cummax(jnp.where(change, place, 0), axis=0)[reach:]
    here = place[reach:]
    total = bias[:, None] + kernel[reach][:, None] * values[:, reach:].astype(jnp.float32)
    for back in range(1, taps):
        piece = values[:, reach - back : length - back].astype(jnp.float32)
        keep = here - back >= begins
        total = total + kernel[reach - back][:, None] * jnp.where(keep[None, :], piece, 0.0)
    return total


def plain_body(tokens, segments, w_lin, w_gate, w_out, conv_kernel, conv_bias, norm_gain, norm_bias):
    rows = tokens[0]
    doc_ids = segments[0]
    count = rows.shape[0]
    reach = conv_kernel.shape[0] - 1
    first = jnp.einsum(
        "rc,tr->ct",
        lax.all_gather(w_lin, "dp", axis=0, tiled=True),
        rows,
        preferred_element_type=jnp.float32,
    )
    second = jnp.einsum(
        "rc,tr->ct",
        lax.all_gather(w_gate, "dp", axis=0, tiled=True),
        rows,
        preferred_element_type=jnp.float32,
    )
    glu = (first * jax.nn.sigmoid(second)).astype(jnp.bfloat16)
    tail, tail_ids = from_behind((glu[:, count - reach :], doc_ids[count - reach :]), "sp", 1)
    extended = jnp.concatenate([tail, glu], axis=1)
    first_block = lax.axis_index("sp") == 0
    ext_ids = jnp.concatenate([jnp.where(first_block, -1, tail_ids), doc_ids], axis=0)
    conv = conv_doc(extended, ext_ids, conv_kernel, conv_bias)
    conved = lax.optimization_barrier(conv.astype(jnp.bfloat16))
    values = conved.astype(jnp.float32)
    mean = jnp.mean(values, axis=0, keepdims=True)
    var = jnp.mean(jnp.square(values - mean), axis=0, keepdims=True)
    normed = (values - mean) * lax.rsqrt(var + 1e-05) * norm_gain[:, None] + norm_bias[:, None]
    act = jax.nn.silu(normed).astype(jnp.bfloat16)
    mixed_out = jnp.einsum(
        "ct,cr->tr",
        act,
        lax.all_gather(w_out, "dp", axis=1, tiled=True),
        preferred_element_type=jnp.float32,
    ).astype(jnp.bfloat16)
    return mixed_out[None]


def kernel(
    n_sp, n_dp, tok_hbm, seg_ref, lin_hbm, gate_hbm, wout_hbm, ck_ref, cb_ref, ng_ref, nb_ref,
    out_ref,
    tok, segh, segx, cnt, buf, glu, conv, act,
    l_sem, h_send, h_recv, o_send, o_recv, y_send, y_recv, z_send, z_recv, x_send, x_recv,
    c_send, c_recv,
):
    rows_, depth = tok_hbm.shape
    shard = lin_hbm.shape[0]
    width = lin_hbm.shape[1]
    ocols = wout_hbm.shape[1]
    taps = ck_ref.shape[0]
    reach = taps - 1
    halo = 32
    full = rows_ + halo
    chunks = width // BLK
    hpb = shard // BLK
    n_lg = 2 * chunks * hpb
    n_wo = (width // BLK) * (ocols // BLK)
    n_units = n_lg + n_wo
    steps = n_units // 3
    wo_base = 2 * chunks * depth

    sp = lax.axis_index("sp")
    dp = lax.axis_index("dp")
    xb = lax.rem(sp, 2)
    zb = lax.rem(sp // 2, 2)
    x_dev = (sp + 1 - 2 * xb, dp)
    z_dev = (sp + 2 - 4 * zb, dp)
    ydp = lax.rem(dp + 2, n_dp)
    y_dev = (sp, ydp)
    c_dev = (sp, dp + 1 - 2 * lax.rem(dp, 2))
    nxt = (lax.rem(sp + 1, n_sp), dp)
    prv = (lax.rem(sp + n_sp - 1, n_sp), dp)
    own_c = zb * 2 + (1 - zb) * xb
    zrc_c = zb * xb + (1 - zb) * 2
    xrc_c = 1 - xb

    def lg_row(s, c, m, h):
        return (2 * c + m) * depth + s * shard + h * BLK

    def unit_row(s, u):
        w = u // n_lg
        lg = (u // hpb) * depth + s * shard + lax.rem(u, hpb) * BLK
        wo = wo_base + s * n_wo * BLK + (u - n_lg) * BLK
        return pl.multiple_of((1 - w) * lg + w * wo, BLK)

    locals_ = []
    for c in range(chunks):
        for m, src in enumerate((lin_hbm, gate_hbm)):
            row = pl.multiple_of(lg_row(dp, c, m, 0), BLK)
            cp = pltpu.make_async_copy(
                src.at[:, pl.ds(c * BLK, BLK)], buf.at[pl.ds(row, shard), :], l_sem.at[len(locals_)]
            )
            cp.start()
            locals_.append((cp, row, shard))
    for h in range(ocols // BLK):
        row = pl.multiple_of(wo_base + dp * n_wo * BLK + h * width, BLK)
        cp = pltpu.make_async_copy(
            wout_hbm.at[:, pl.ds(h * BLK, BLK)], buf.at[pl.ds(row, width), :], l_sem.at[len(locals_)]
        )
        cp.start()
        locals_.append((cp, row, width))
    tcp = pltpu.make_async_copy(
        tok_hbm, tok.at[pl.ds(halo, rows_), :], l_sem.at[len(locals_)]
    )
    tcp.start()

    barrier = pltpu.get_barrier_semaphore()
    for dev in (x_dev, z_dev, y_dev, c_dev, nxt, prv):
        pl.semaphore_signal(barrier, inc=1, device_id=dev, device_id_type=MESH)
    pl.semaphore_wait(barrier, 6)

    def rcopy(src, dst, ss, rs, dev):
        return pltpu.make_async_remote_copy(
            src_ref=src, dst_ref=dst, send_sem=ss, recv_sem=rs, device_id=dev, device_id_type=MESH
        )

    sends = []
    seg_cp = rcopy(seg_ref.at[:, pl.ds(rows_ - LANES, LANES)], segh, h_send.at[1], h_recv.at[1], nxt)
    seg_cp.start()
    tok_cp = rcopy(
        tok_hbm.at[pl.ds(rows_ - halo, halo), :], tok.at[pl.ds(0, halo), :], h_send.at[0], h_recv.at[0], nxt
    )
    tok_cp.start()
    sends += [seg_cp, tok_cp]

    def ucopy(s, u, ss, rs, dev):
        row = unit_row(s, u)
        ref = buf.at[pl.ds(row, BLK), :]
        return rcopy(ref, ref, ss, rs, dev)

    ydone = 0
    owns = []
    for n, (cp, row, size) in enumerate(locals_):
        cp.wait()
        if n < 2 * chunks:
            have = (n + 1) * hpb
        else:
            have = n_lg + (n + 1 - 2 * chunks) * (width // BLK)
        while ydone < steps and 3 * ydone + 2 < have:
            yc = ucopy(dp, 3 * ydone + own_c, y_send.at[ydone], y_recv.at[ydone], y_dev)
            yc.start()
            sends.append(yc)
            ydone += 1
        ref = buf.at[pl.ds(row, size), :]
        oc = rcopy(ref, ref, o_send.at[n], o_recv.at[n], c_dev)
        oc.start()
        sends.append(oc)
        owns.append(oc)

    def forward(i, kind, color):
        cc = ucopy(ydp, 3 * i + color, c_send.at[3 * i + kind], c_recv.at[3 * i + kind], c_dev)
        cc.start()
        sends.append(cc)

    fwd = {}

    def y_copy(i):
        return ucopy(dp, 3 * i + own_c, y_send.at[i], y_recv.at[i], y_dev)

    def stage_y(i):
        ucopy(ydp, 3 * i + own_c, y_send.at[i], y_recv.at[i], y_dev).wait_recv()
        zc = ucopy(ydp, 3 * i + own_c, z_send.at[i], z_recv.at[i], z_dev)
        zc.start()
        xc = ucopy(ydp, 3 * i + xb, x_send.at[i], x_recv.at[i], x_dev)

        @pl.when(zb == 0)
        def _():
            xc.start()

        sends.append(zc)
        sends.append(xc)
        forward(i, 0, own_c)

    def stage_z(i):
        ucopy(ydp, 3 * i + zrc_c, z_send.at[i], z_recv.at[i], z_dev).wait_recv()
        xc = ucopy(ydp, 3 * i + xb, x_send.at[i], x_recv.at[i], x_dev)

        @pl.when(zb == 1)
        def _():
            xc.start()

        forward(i, 1, zrc_c)

    def stage_x(i):
        ucopy(ydp, 3 * i + xrc_c, x_send.at[i], x_recv.at[i], x_dev).wait_recv()
        forward(i, 2, xrc_c)

    cdp = ydp + 1 - 2 * lax.rem(ydp, 2)
    waited = set()

    def core_wait(i):
        if i in waited:
            return
        waited.add(i)
        for kind, color in enumerate((own_c, zrc_c, xrc_c)):
            ucopy(cdp, 3 * i + color, c_send.at[3 * i + kind], c_recv.at[3 * i + kind], c_dev).wait_recv()

    def tick(n):
        if 0 <= n < steps:
            stage_y(n)
        if 0 <= n - 2 < steps:
            stage_z(n - 2)
        if 0 <= n - 3 < steps:
            stage_x(n - 3)

    def count_rows():
        seg_cp.wait_recv()
        before = jnp.where(sp == 0, -1, segh[...])[:, LANES - halo :]
        line = jnp.concatenate([before, seg_ref[...]], axis=1)
        pad = 640 - full
        line = jnp.concatenate([line, jnp.zeros((1, pad), jnp.int32)], axis=1) if pad else line
        tall = jnp.transpose(jnp.broadcast_to(line, (LANES, line.shape[1])))
        segx[...] = tall[:full]

        def one(r, carry):
            base = pl.multiple_of(r * 64, 64)
            here = segx[pl.ds(base + halo, 64), :]
            total = jnp.zeros((64, LANES), jnp.int32)
            for k in range(1, taps):
                total = total + (segx[pl.ds(base + halo - k, 64), :] == here).astype(jnp.int32)
            cnt[pl.ds(base, 64), :] = total
            return carry

        lax.fori_loop(0, rows_ // 64, one, 0)

    def project(c):
        for m in range(2):
            owns[2 * c + m].wait_recv()
        lin = jnp.dot(
            tok[...], buf[pl.ds(2 * c * depth, depth), :], preferred_element_type=jnp.float32
        )
        gate = jnp.dot(
            tok[...], buf[pl.ds((2 * c + 1) * depth, depth), :], preferred_element_type=jnp.float32
        )
        val = (lin * (1.0 / (1.0 + jnp.exp(-gate)))).astype(jnp.bfloat16).astype(jnp.float32)
        for h in range(BLK // LANES):
            glu[c * (BLK // LANES) + h] = val[:, h * LANES : (h + 1) * LANES]

    RT = 64

    def convolve(c):
        for h in range(BLK // LANES):
            g = c * (BLK // LANES) + h
            lanes = pl.ds(g * LANES, LANES)

            def one(r, carry):
                base = pl.multiple_of(r * RT, RT)
                valid = cnt[pl.ds(base, RT), :]
                total = cb_ref[:, lanes] + ck_ref[pl.ds(reach, 1), lanes] * glu[g, pl.ds(base + halo, RT), :]
                for k in range(1, taps):
                    piece = glu[g, pl.ds(base + halo - k, RT), :]
                    total = total + ck_ref[pl.ds(reach - k, 1), lanes] * jnp.where(valid >= k, piece, 0.0)
                conv[pl.ds(base, RT), lanes] = total.astype(jnp.bfloat16)
                return carry

            lax.fori_loop(0, rows_ // RT, one, 0)

    def normalise():
        def one(r, carry):
            base = pl.multiple_of(r * 32, 32)
            v = conv[pl.ds(base, 32), :].astype(jnp.float32)
            mean = jnp.mean(v, axis=1, keepdims=True)
            dev = v - mean
            var = jnp.mean(dev * dev, axis=1, keepdims=True)
            nrm = dev * lax.rsqrt(var + 1e-05) * ng_ref[...] + nb_ref[...]
            act[pl.ds(base, 32), :] = (nrm / (1.0 + jnp.exp(-nrm))).astype(jnp.bfloat16)
            return carry

        lax.fori_loop(0, rows_ // 32, one, 0)

    def emit(s, h):
        row = wo_base + s * n_wo * BLK + h * width
        out_ref[:, pl.ds(s * ocols + h * BLK, BLK)] = jnp.dot(
            act[...], buf[pl.ds(row, width), :], preferred_element_type=jnp.float32
        ).astype(jnp.bfloat16)

    ready = 0
    tick(0)
    count_rows()
    tcp.wait()
    tok_cp.wait_recv()
    at = 1
    for c in range(chunks):
        need = (2 * hpb * (c + 1) - 1) // 3
        while at <= need + 3:
            tick(at)
            at += 1
        for i in range(ready, need + 1):
            core_wait(i)
        ready = need + 1
        project(c)
        tick(at)
        at += 1
        convolve(c)
    while at <= steps + 2:
        tick(at)
        at += 1
    normalise()
    for i in range(ready, steps):
        core_wait(i)
    for h in range(ocols // BLK):
        owns[2 * chunks + h].wait_recv()
    for s in range(n_dp):
        for h in range(ocols // BLK):
            emit(s, h)
    for cp in sends:
        cp.wait_send()


def fast_body(n_sp, n_dp, tokens, segments, w_lin, w_gate, w_out, conv_kernel, conv_bias, norm_gain, norm_bias):
    rows, depth = tokens.shape[1:]
    width = w_lin.shape[1]
    ocols = w_out.shape[1]
    units = (2 * w_lin.shape[0] * width + width * ocols) // (BLK * BLK)
    steps = units // 3
    n_local = 2 * (width // BLK) + ocols // BLK
    vm = pl.BlockSpec(memory_space=pltpu.VMEM)
    hb = pl.BlockSpec(memory_space=pl.ANY)
    dma = pltpu.SemaphoreType.DMA
    out = pl.pallas_call(
        functools.partial(kernel, n_sp, n_dp),
        out_shape=jax.ShapeDtypeStruct((rows, ocols * n_dp), jnp.bfloat16),
        in_specs=[hb, vm, hb, hb, hb, vm, vm, vm, vm],
        out_specs=vm,
        scratch_shapes=[
            pltpu.VMEM((rows + 32, depth), jnp.bfloat16),
            pltpu.VMEM((1, LANES), jnp.int32),
            pltpu.VMEM((rows + 32, LANES), jnp.int32),
            pltpu.VMEM((rows, LANES), jnp.int32),
            pltpu.VMEM((units * n_dp * BLK, BLK), jnp.bfloat16),
            pltpu.VMEM((width // LANES, rows + 32, LANES), jnp.float32),
            pltpu.VMEM((rows, width), jnp.bfloat16),
            pltpu.VMEM((rows, width), jnp.bfloat16),
            dma((n_local + 1,)),
            dma((2,)),
            dma((2,)),
            dma((n_local,)),
            dma((n_local,)),
            dma((steps,)),
            dma((steps,)),
            dma((steps,)),
            dma((steps,)),
            dma((steps,)),
            dma((steps,)),
            dma((steps * 3,)),
            dma((steps * 3,)),
        ],
        compiler_params=pltpu.CompilerParams(
            collective_id=0, has_side_effects=True, vmem_limit_bytes=60 * 1024 * 1024
        ),
    )(
        tokens[0], segments, w_lin, w_gate, w_out, conv_kernel,
        conv_bias[None], norm_gain[None], norm_bias[None],
    )
    return out[None]


def solution(mesh):
    placed = (
        P("dp", "sp", None),
        P("dp", "sp"),
        P("dp", None),
        P("dp", None),
        P(None, "dp"),
        P(),
        P(),
        P(),
        P(),
    )
    n_sp, n_dp = mesh.shape["sp"], mesh.shape["dp"]
    body = functools.partial(fast_body, n_sp, n_dp) if n_dp == 4 and n_sp % 4 == 0 else plain_body
    return jax.shard_map(
        body, mesh=mesh, in_specs=placed, out_specs=P("dp", "sp", None), check_vma=False
    )
```

```python
import functools

import jax
import jax.numpy as jnp
from jax import lax
from jax.experimental import pallas as pl
from jax.experimental.pallas import tpu as pltpu
from jax.sharding import PartitionSpec as P

MESH = pl.DeviceIdType.MESH
BLK = 256
LANES = 128
UB = 128
VMEM_MAX = 67043328
SPARE = 512 * 1024
RT = 64
SKEW_Z = 3
SKEW_X = 6


def from_behind(value, axis, by):
    devices = lax.axis_size(axis)
    pairs = [(i, i + by) for i in range(devices) if 0 <= i + by < devices]
    return lax.ppermute(value, axis, pairs)


def conv_doc(values, doc_ids, kernel, bias):
    taps = kernel.shape[0]
    reach = taps - 1
    length = values.shape[1]
    place = lax.iota(jnp.int32, length)
    change = jnp.concatenate([jnp.ones((1,), jnp.bool_), doc_ids[1:] != doc_ids[:-1]])
    begins = lax.cummax(jnp.where(change, place, 0), axis=0)[reach:]
    here = place[reach:]
    total = bias[:, None] + kernel[reach][:, None] * values[:, reach:].astype(jnp.float32)
    for back in range(1, taps):
        piece = values[:, reach - back : length - back].astype(jnp.float32)
        keep = here - back >= begins
        total = total + kernel[reach - back][:, None] * jnp.where(keep[None, :], piece, 0.0)
    return total


def plain_body(tokens, segments, w_lin, w_gate, w_out, conv_kernel, conv_bias, norm_gain, norm_bias):
    rows = tokens[0]
    doc_ids = segments[0]
    count = rows.shape[0]
    reach = conv_kernel.shape[0] - 1
    first = jnp.einsum(
        "rc,tr->ct",
        lax.all_gather(w_lin, "dp", axis=0, tiled=True),
        rows,
        preferred_element_type=jnp.float32,
    )
    second = jnp.einsum(
        "rc,tr->ct",
        lax.all_gather(w_gate, "dp", axis=0, tiled=True),
        rows,
        preferred_element_type=jnp.float32,
    )
    glu = (first * jax.nn.sigmoid(second)).astype(jnp.bfloat16)
    tail, tail_ids = from_behind((glu[:, count - reach :], doc_ids[count - reach :]), "sp", 1)
    extended = jnp.concatenate([tail, glu], axis=1)
    first_block = lax.axis_index("sp") == 0
    ext_ids = jnp.concatenate([jnp.where(first_block, -1, tail_ids), doc_ids], axis=0)
    conv = conv_doc(extended, ext_ids, conv_kernel, conv_bias)
    conved = lax.optimization_barrier(conv.astype(jnp.bfloat16))
    values = conved.astype(jnp.float32)
    mean = jnp.mean(values, axis=0, keepdims=True)
    var = jnp.mean(jnp.square(values - mean), axis=0, keepdims=True)
    normed = (values - mean) * lax.rsqrt(var + 1e-05) * norm_gain[:, None] + norm_bias[:, None]
    act = jax.nn.silu(normed).astype(jnp.bfloat16)
    mixed_out = jnp.einsum(
        "ct,cr->tr",
        act,
        lax.all_gather(w_out, "dp", axis=1, tiled=True),
        preferred_element_type=jnp.float32,
    ).astype(jnp.bfloat16)
    return mixed_out[None]


def kernel(
    n_sp, n_dp, tok_hbm, seg_ref, lin_hbm, gate_hbm, wout_hbm, ck_ref, cb_ref, ng_ref, nb_ref,
    out_ref,
    tok, segh, segx, cnt, buf, glu, conv, act,
    l_sem, h_send, h_recv, o_send, o_recv, y_send, y_recv, z_send, z_recv, x_send, x_recv,
    c_send, c_recv,
):
    rows_, depth = tok_hbm.shape
    shard = lin_hbm.shape[0]
    width = lin_hbm.shape[1]
    ocols = wout_hbm.shape[1]
    taps = ck_ref.shape[0]
    reach = taps - 1
    halo = 32
    full = rows_ + halo
    chunks = width // BLK
    hpb = shard // UB
    n_lg = 2 * chunks * hpb
    n_wo = (width // UB) * (ocols // BLK)
    n_units = n_lg + n_wo
    steps = n_units // 3
    wo_base = 2 * chunks * depth

    sp = lax.axis_index("sp")
    dp = lax.axis_index("dp")
    xb = lax.rem(sp, 2)
    zb = lax.rem(sp // 2, 2)
    x_dev = (sp + 1 - 2 * xb, dp)
    z_dev = (sp + 2 - 4 * zb, dp)
    ydp = lax.rem(dp + 2, n_dp)
    y_dev = (sp, ydp)
    c_dev = (sp, dp + 1 - 2 * lax.rem(dp, 2))
    nxt = (lax.rem(sp + 1, n_sp), dp)
    prv = (lax.rem(sp + n_sp - 1, n_sp), dp)
    own_c = zb * 2 + (1 - zb) * xb
    zrc_c = zb * xb + (1 - zb) * 2
    xrc_c = 1 - xb

    def lg_row(s, c, m):
        return (2 * c + m) * depth + s * shard

    def unit_row(s, u):
        w = u // n_lg
        lg = (u // hpb) * depth + s * shard + lax.rem(u, hpb) * UB
        wo = wo_base + s * n_wo * UB + (u - n_lg) * UB
        return pl.multiple_of((1 - w) * lg + w * wo, UB)

    locals_ = []
    for c in range(chunks):
        for m, src in enumerate((lin_hbm, gate_hbm)):
            row = pl.multiple_of(lg_row(dp, c, m), UB)
            cp = pltpu.make_async_copy(
                src.at[:, pl.ds(c * BLK, BLK)], buf.at[pl.ds(row, shard), :], l_sem.at[len(locals_)]
            )
            cp.start()
            locals_.append((cp, row, shard))
    for h in range(ocols // BLK):
        row = pl.multiple_of(wo_base + dp * n_wo * UB + h * width, UB)
        cp = pltpu.make_async_copy(
            wout_hbm.at[:, pl.ds(h * BLK, BLK)], buf.at[pl.ds(row, width), :], l_sem.at[len(locals_)]
        )
        cp.start()
        locals_.append((cp, row, width))
    tcp = pltpu.make_async_copy(
        tok_hbm, tok.at[pl.ds(halo, rows_), :], l_sem.at[len(locals_)]
    )
    tcp.start()

    barrier = pltpu.get_barrier_semaphore()
    for dev in (x_dev, z_dev, y_dev, c_dev, nxt, prv):
        pl.semaphore_signal(barrier, inc=1, device_id=dev, device_id_type=MESH)
    pl.semaphore_wait(barrier, 6)

    def rcopy(src, dst, ss, rs, dev):
        return pltpu.make_async_remote_copy(
            src_ref=src, dst_ref=dst, send_sem=ss, recv_sem=rs, device_id=dev, device_id_type=MESH
        )

    sends = []
    seg_cp = rcopy(seg_ref.at[:, pl.ds(rows_ - LANES, LANES)], segh, h_send.at[1], h_recv.at[1], nxt)
    seg_cp.start()
    tok_cp = rcopy(
        tok_hbm.at[pl.ds(rows_ - halo, halo), :], tok.at[pl.ds(0, halo), :], h_send.at[0], h_recv.at[0], nxt
    )
    tok_cp.start()
    sends += [seg_cp, tok_cp]

    def ucopy(s, u, ss, rs, dev):
        row = unit_row(s, u)
        ref = buf.at[pl.ds(row, UB), :]
        return rcopy(ref, ref, ss, rs, dev)

    ydone = 0
    owns = []
    for n, (cp, row, size) in enumerate(locals_):
        cp.wait()
        if n < 2 * chunks:
            have = (n + 1) * hpb
        else:
            have = n_lg + (n + 1 - 2 * chunks) * (width // UB)
        while ydone < steps and 3 * ydone + 2 < have:
            yc = ucopy(dp, 3 * ydone + own_c, y_send.at[ydone], y_recv.at[ydone], y_dev)
            yc.start()
            sends.append(yc)
            ydone += 1
        ref = buf.at[pl.ds(row, size), :]
        oc = rcopy(ref, ref, o_send.at[n], o_recv.at[n], c_dev)
        oc.start()
        sends.append(oc)
        owns.append(oc)

    def forward(i, kind, color):
        cc = ucopy(ydp, 3 * i + color, c_send.at[3 * i + kind], c_recv.at[3 * i + kind], c_dev)
        cc.start()
        sends.append(cc)

    fwd = {}

    def y_copy(i):
        return ucopy(dp, 3 * i + own_c, y_send.at[i], y_recv.at[i], y_dev)

    def stage_y(i):
        ucopy(ydp, 3 * i + own_c, y_send.at[i], y_recv.at[i], y_dev).wait_recv()
        zc = ucopy(ydp, 3 * i + own_c, z_send.at[i], z_recv.at[i], z_dev)
        zc.start()
        xc = ucopy(ydp, 3 * i + xb, x_send.at[i], x_recv.at[i], x_dev)

        @pl.when(zb == 0)
        def _():
            xc.start()

        sends.append(zc)
        sends.append(xc)
        forward(i, 0, own_c)

    def stage_z(i):
        ucopy(ydp, 3 * i + zrc_c, z_send.at[i], z_recv.at[i], z_dev).wait_recv()
        xc = ucopy(ydp, 3 * i + xb, x_send.at[i], x_recv.at[i], x_dev)

        @pl.when(zb == 1)
        def _():
            xc.start()

        forward(i, 1, zrc_c)

    def stage_x(i):
        ucopy(ydp, 3 * i + xrc_c, x_send.at[i], x_recv.at[i], x_dev).wait_recv()
        forward(i, 2, xrc_c)

    cdp = ydp + 1 - 2 * lax.rem(ydp, 2)
    waited = set()

    def core_wait(i):
        if i in waited:
            return
        waited.add(i)
        for kind, color in enumerate((own_c, zrc_c, xrc_c)):
            ucopy(cdp, 3 * i + color, c_send.at[3 * i + kind], c_recv.at[3 * i + kind], c_dev).wait_recv()

    def tick(n):
        if 0 <= n < steps:
            stage_y(n)
        if 0 <= n - SKEW_Z < steps:
            stage_z(n - SKEW_Z)
        if 0 <= n - SKEW_X < steps:
            stage_x(n - SKEW_X)

    def count_rows():
        seg_cp.wait_recv()
        before = jnp.where(sp == 0, -1, segh[...])[:, LANES - halo :]
        line = jnp.concatenate([before, seg_ref[...]], axis=1)
        pad = 640 - full
        line = jnp.concatenate([line, jnp.zeros((1, pad), jnp.int32)], axis=1) if pad else line
        tall = jnp.transpose(jnp.broadcast_to(line, (LANES, line.shape[1])))
        segx[...] = tall[:full]

        def one(r, carry):
            base = pl.multiple_of(r * 64, 64)
            here = segx[pl.ds(base + halo, 64), :]
            total = jnp.zeros((64, LANES), jnp.int32)
            for k in range(1, taps):
                total = total + (segx[pl.ds(base + halo - k, 64), :] == here).astype(jnp.int32)
            cnt[pl.ds(base, 64), :] = total
            return carry

        lax.fori_loop(0, rows_ // 64, one, 0)

    def project(c):
        for m in range(2):
            owns[2 * c + m].wait_recv()
        lin = jnp.dot(
            tok[...], buf[pl.ds(2 * c * depth, depth), :], preferred_element_type=jnp.float32
        )
        gate = jnp.dot(
            tok[...], buf[pl.ds((2 * c + 1) * depth, depth), :], preferred_element_type=jnp.float32
        )
        val = (lin * (0.5 + 0.5 * jnp.tanh(0.5 * gate))).astype(jnp.bfloat16).astype(jnp.float32)
        for h in range(BLK // LANES):
            glu[c * (BLK // LANES) + h] = val[:, h * LANES : (h + 1) * LANES]

    def convolve(c, part, parts):
        groups = [c * (BLK // LANES) + h for h in range(BLK // LANES)]

        def one(r, carry):
            base = pl.multiple_of(part * (rows_ // parts) + r * RT, RT)
            valid = cnt[pl.ds(base, RT), :]
            lanes = [pl.ds(g * LANES, LANES) for g in groups]
            totals = [
                cb_ref[:, ln] + ck_ref[pl.ds(reach, 1), ln] * glu[g, pl.ds(base + halo, RT), :]
                for g, ln in zip(groups, lanes)
            ]
            for k in range(1, taps):
                keep = valid >= k
                for n, (g, ln) in enumerate(zip(groups, lanes)):
                    piece = jnp.where(keep, glu[g, pl.ds(base + halo - k, RT), :], 0.0)
                    totals[n] = totals[n] + ck_ref[pl.ds(reach - k, 1), ln] * piece
            for ln, total in zip(lanes, totals):
                conv[pl.ds(base, RT), ln] = total.astype(jnp.bfloat16)
            return carry

        lax.fori_loop(0, rows_ // parts // RT, one, 0)

    def normalise(part, parts):
        each = rows_ // parts // 32

        def one(r, carry):
            base = pl.multiple_of(part * (rows_ // parts) + r * 32, 32)
            v = conv[pl.ds(base, 32), :].astype(jnp.float32)
            mean = jnp.mean(v, axis=1, keepdims=True)
            dev = v - mean
            var = jnp.mean(dev * dev, axis=1, keepdims=True)
            nrm = dev * lax.rsqrt(var + 1e-05) * ng_ref[...] + nb_ref[...]
            act[pl.ds(base, 32), :] = (nrm * (0.5 + 0.5 * jnp.tanh(0.5 * nrm))).astype(jnp.bfloat16)
            return carry

        lax.fori_loop(0, each, one, 0, unroll=2)

    def emit(s, h):
        row = pl.multiple_of(wo_base + s * n_wo * UB + h * width, UB)
        at_col = pl.multiple_of(s * ocols + h * BLK, BLK)
        out_ref[:, pl.ds(at_col, BLK)] = jnp.dot(
            act[...], buf[pl.ds(row, width), :], preferred_element_type=jnp.float32
        ).astype(jnp.bfloat16)

    state = {"at": 0, "ready": 0}

    def advance(upto=None):
        goal = state["at"] if upto is None else upto
        while state["at"] <= min(goal, steps - 1 + SKEW_X):
            tick(state["at"])
            state["at"] += 1

    def all_from_core(need):
        for i in range(state["ready"], need + 1):
            core_wait(i)
        state["ready"] = max(state["ready"], need + 1)

    advance(0)
    count_rows()
    tcp.wait()
    tok_cp.wait_recv()
    for c in range(chunks):
        need = (2 * hpb * (c + 1) - 1) // 3
        advance(need + SKEW_X)
        all_from_core(need)
        project(c)
        advance()
        for h in range(2):
            convolve(c, h, 2)
            advance()
    normalise(0, 2)
    advance()
    normalise(1, 2)
    advance()
    heads = ocols // BLK
    for h in range(heads):
        owns[2 * chunks + h].wait_recv()
        emit(dp, h)
        emit(dp + 1 - 2 * lax.rem(dp, 2), h)
        advance()
    for h in range(heads):
        need = (n_lg + (h + 1) * (width // UB) - 1) // 3
        advance(need + SKEW_X)
        emit(ydp, h)
        all_from_core(need)
        emit(cdp, h)
    for cp in sends:
        cp.wait_send()


def fast_body(n_sp, n_dp, tokens, segments, w_lin, w_gate, w_out, conv_kernel, conv_bias, norm_gain, norm_bias):
    rows, depth = tokens.shape[1:]
    width = w_lin.shape[1]
    ocols = w_out.shape[1]
    units = (2 * w_lin.shape[0] * width + width * ocols) // (BLK * UB)
    steps = units // 3
    n_local = 2 * (width // BLK) + ocols // BLK
    vm = pl.BlockSpec(memory_space=pltpu.VMEM)
    hb = pl.BlockSpec(memory_space=pltpu.HBM)
    dma = pltpu.SemaphoreType.DMA
    out = pl.pallas_call(
        functools.partial(kernel, n_sp, n_dp),
        out_shape=pltpu.VMEM((rows, ocols * n_dp), jnp.bfloat16),
        in_specs=[hb, vm, hb, hb, hb, vm, vm, vm, vm],
        out_specs=vm,
        scratch_shapes=[
            pltpu.VMEM((rows + 32, depth), jnp.bfloat16),
            pltpu.VMEM((1, LANES), jnp.int32),
            pltpu.VMEM((rows + 32, LANES), jnp.int32),
            pltpu.VMEM((rows, LANES), jnp.int32),
            pltpu.VMEM((units * n_dp * UB, BLK), jnp.bfloat16),
            pltpu.VMEM((width // LANES, rows + 32, LANES), jnp.float32),
            pltpu.VMEM((rows, width), jnp.bfloat16),
            pltpu.VMEM((rows, width), jnp.bfloat16),
            dma((n_local + 1,)),
            dma((2,)),
            dma((2,)),
            dma((n_local,)),
            dma((n_local,)),
            dma((steps,)),
            dma((steps,)),
            dma((steps,)),
            dma((steps,)),
            dma((steps,)),
            dma((steps,)),
            dma((steps * 3,)),
            dma((steps * 3,)),
        ],
        compiler_params=pltpu.CompilerParams(
            collective_id=0, has_side_effects=True, vmem_limit_bytes=VMEM_MAX - rows * ocols * n_dp * 2 - SPARE
        ),
    )(
        tokens[0], segments, w_lin, w_gate, w_out, conv_kernel,
        conv_bias[None], norm_gain[None], norm_bias[None],
    )
    return out[None]


def solution(mesh):
    placed = (
        P("dp", "sp", None),
        P("dp", "sp"),
        P("dp", None),
        P("dp", None),
        P(None, "dp"),
        P(),
        P(),
        P(),
        P(),
    )
    n_sp, n_dp = mesh.shape["sp"], mesh.shape["dp"]
    body = functools.partial(fast_body, n_sp, n_dp) if n_dp == 4 and n_sp % 4 == 0 else plain_body
    return jax.shard_map(
        body, mesh=mesh, in_specs=placed, out_specs=P("dp", "sp", None), check_vma=False
    )
```
